128 devices in a mesh: fs: 32 (over z, y, core), tp: 4 (over x).
Axes of the slice: x: 4, y: 4, z: 4, core: 2. Of those that a mesh axis runs over, the one named last changes fastest.
Arguments:
- x_saved: bfloat16 [65536, 2048], P('fs'), may hold values from -6 to 6
- h_saved: bfloat16 [65536, 1024], P('fs', 'tp'), may hold values from -6 to 6
- key_cot: bfloat16 [65536, 1024], P('fs', 'tp'), may hold values from -6 to 6
- value_cot: bfloat16 [65536, 1024], P('fs', 'tp'), may hold values from -6 to 6
- out_cot: bfloat16 [65536, 2048], P('fs'), may hold values from -6 to 6
- w_key: float32 [2048, 1024], P('fs', 'tp'), may hold values from -0.125 to 0.125
- w_value: float32 [2048, 1024], P('fs', 'tp'), may hold values from -0.125 to 0.125
- w_out: float32 [1024, 2048], P('tp', 'fs'), may hold values from -0.1875 to 0.1875
- p_key: bfloat16 [2048, 256], P('fs'), may hold values from -1 to 1, as said below
- p_value: bfloat16 [2048, 256], P('fs'), may hold values from -1 to 1, as said below
- p_out: bfloat16 [2048, 256], P('fs'), may hold values from -1 to 1, as said below
- m_key: float32 [2, 256, 1024], P(None, 'fs', 'tp'), may hold values from -1.5 to 1.5, as said below
- m_value: float32 [2, 256, 1024], P(None, 'fs', 'tp'), may hold values from -1.5 to 1.5, as said below
- m_out: float32 [2, 256, 1024], P(None, 'fs', 'tp'), may hold values from -1.5 to 1.5, as said below
Outputs:
- step_key: float32 [2048, 1024], P('fs', 'tp')
- step_value: float32 [2048, 1024], P('fs', 'tp')
- step_out: float32 [1024, 2048], P('tp', 'fs')
- copy_key: bfloat16 [2048, 1024], P(None, 'tp')
- copy_value: bfloat16 [2048, 1024], P(None, 'tp')
- copy_out: bfloat16 [1024, 2048], P('tp')
- new_m_key: float32 [2, 256, 1024], P(None, 'fs', 'tp')
- new_m_value: float32 [2, 256, 1024], P(None, 'fs', 'tp')
- new_m_out: float32 [2, 256, 1024], P(None, 'fs', 'tp')
The draws below stay inside these ranges and needn't reach their ends.
Inputs may be any that keep to these rules, and one draw needn't show every extreme that they name: `p_key`: factor entries are real-valued, dense and of full rank. `p_value`: factor entries are real-valued, dense and of full rank. `p_out`: factor entries are real-valued, dense and of full rank. `m_key`: plane 1 (second moments) lies in 0.05 to 1. `m_value`: plane 1 (second moments) lies in 0.05 to 1. `m_out`: plane 1 (second moments) lies in 0.05 to 1.
All inputs are finite; a program needn't handle non-finite values.
Results may differ from the reference program's by a relative error of at most 0.0085.
Values may be sent and summed in bfloat16 or wider, within the bound.
A program may use at most 128 MiB of HBM per device.

```python
import math
import jax
import jax.numpy as jnp
from jax import lax

D = 2048
HW = 1024
RANK = 256
TOKENS = 65536


def factor_draw(key, member):
    key = jax.random.fold_in(key, member)
    key_base, key_cols = jax.random.split(key, 2)
    gaussian = jax.random.truncated_normal(key_base, -4.0, 4.0, (D, RANK), jnp.float32)
    columns = jnp.arange(RANK, dtype=jnp.float32)
    rising = 10.0 ** (columns / RANK) * jax.random.uniform(key_cols, (RANK,), jnp.float32, 0.7, 1.4)
    factor_values = gaussian * rising[None, :] * D ** (-0.5)
    return jnp.clip(factor_values, -1.0, 1.0).astype(jnp.bfloat16)


def moment_draw(key, member):
    key = jax.random.fold_in(key, member)
    key_one, key_two = jax.random.split(key)
    plane_one = 0.3 * jax.random.truncated_normal(key_one, -5.0, 5.0, (RANK, HW), jnp.float32)
    plane_two = jnp.exp(jax.random.uniform(key_two, (RANK, HW), jnp.float32, math.log(0.05), 0.0))
    return jnp.stack([plane_one, plane_two]).astype(jnp.float32)


def draw_p_key(key, part):
    return factor_draw(key, 11)


def draw_p_value(key, part):
    return factor_draw(key, 12)


def draw_p_out(key, part):
    return factor_draw(key, 13)


def draw_m_key(key, part):
    return moment_draw(key, 21)


def draw_m_value(key, part):
    return moment_draw(key, 22)


def draw_m_out(key, part):
    return moment_draw(key, 23)


def block_levels(rng, dims, pieces, smallest, top_value):
    def one(position, parts):
        draws = jax.random.uniform(jax.random.fold_in(jax.random.fold_in(rng, 6), position), (parts,), jnp.float32, smallest / len(pieces), top_value / len(pieces))
        return jnp.repeat(jnp.exp(draws), dims[position] // parts).reshape((-1,) + (1,) * (len(dims) - position - 1))

    loudness = one(*pieces[0])
    for cut in pieces[1:]:
        loudness = loudness * one(*cut)
    return loudness


def normal_values(key, extent, width, limit, cuts=(), kind=jnp.bfloat16):
    values = jax.random.normal(key, extent, jnp.float32) * width
    if len(cuts) > 0:
        values = block_levels(key, extent, cuts, -0.22, 0.18) * values
    return jnp.clip(values, min=-limit, max=limit).astype(kind)


def setup_inputs(seed: int = 0) -> dict:
    keys = jax.random.split(jax.random.key(seed), 15)
    x_saved = normal_values(keys[0], (TOKENS, D), 1.0, 6.0, ((0, 32),))
    h_saved = normal_values(keys[1], (TOKENS, HW), 1.0, 6.0, ((0, 32), (1, 4)))
    key_cot = normal_values(keys[2], (TOKENS, HW), 1.0, 6.0, ((0, 32), (1, 4)))
    value_cot = normal_values(keys[3], (TOKENS, HW), 1.0, 6.0, ((0, 32), (1, 4)))
    out_cot = normal_values(keys[4], (TOKENS, D), 1.0, 6.0, ((0, 32),))
    w_key = normal_values(keys[5], (D, HW), D ** -0.5, 0.125, ((0, 32), (1, 4)), jnp.float32)
    w_value = normal_values(keys[6], (D, HW), D ** -0.5, 0.125, ((0, 32), (1, 4)), jnp.float32)
    w_out = normal_values(keys[7], (HW, D), HW ** -0.5, 0.1875, ((0, 4), (1, 32)), jnp.float32)
    p_key = draw_p_key(jax.random.fold_in(keys[14], 71), 0)
    p_value = draw_p_value(jax.random.fold_in(keys[14], 71), 0)
    p_out = draw_p_out(jax.random.fold_in(keys[14], 71), 0)
    m_key = draw_m_key(jax.random.fold_in(keys[14], 71), 0)
    m_value = draw_m_value(jax.random.fold_in(keys[14], 71), 0)
    m_out = draw_m_out(jax.random.fold_in(keys[14], 71), 0)
    return dict(x_saved=x_saved, h_saved=h_saved, key_cot=key_cot, value_cot=value_cot, out_cot=out_cot, w_key=w_key, w_value=w_value, w_out=w_out, p_key=p_key, p_value=p_value, p_out=p_out, m_key=m_key, m_value=m_value, m_out=m_out)


beta_one = 0.9
beta_two = 0.9
learn_rate = 0.01

def exact_dot(left, right):
    return jnp.dot(left.astype(jnp.float32), right.astype(jnp.float32), precision=lax.Precision.HIGHEST)

def reference(x_saved, h_saved, key_cot, value_cot, out_cot, w_key, w_value, w_out, p_key, p_value, p_out, m_key, m_value, m_out):
    x_wide = x_saved.astype(jnp.float32).T
    grad_key = exact_dot(x_wide, key_cot)
    grad_value = exact_dot(x_wide, value_cot)
    grad_out_t = exact_dot(out_cot.astype(jnp.float32).T, h_saved)
    factors = (p_key, p_value, p_out)
    projected = [exact_dot(factors[0].astype(jnp.float32).T, grad_key), exact_dot(factors[1].astype(jnp.float32).T, grad_value), exact_dot(factors[2].astype(jnp.float32).T, grad_out_t)]
    total = jnp.sum(projected[0] * projected[0]) + jnp.sum(projected[1] * projected[1]) + jnp.sum(projected[2] * projected[2])
    norm_scale = jnp.sqrt(total / (3 * RANK * HW) + 1e-06)
    olds = (m_key, m_value, m_out)
    steps = []
    moments = []
    for member in range(3):
        normed = projected[member] / norm_scale
        moment_one = beta_one * olds[member][0] + (1 - beta_one) * normed
        moment_two = beta_two * olds[member][1] + (1 - beta_two) * normed * normed
        direction = (moment_one / jnp.sqrt(moment_two)).astype(jnp.bfloat16)
        steps.append(exact_dot(factors[member], direction))
        moments.append(jnp.stack([moment_one, moment_two]))
    step_key = steps[0]
    step_value = steps[1]
    step_out = steps[2].T
    copy_key = (w_key - learn_rate * step_key).astype(jnp.bfloat16)
    copy_value = (w_value - learn_rate * step_value).astype(jnp.bfloat16)
    copy_out = (w_out - learn_rate * step_out).astype(jnp.bfloat16)
    return (step_key, step_value, step_out, copy_key, copy_value, copy_out, moments[0], moments[1], moments[2])
```

```python
import jax
import jax.numpy as jnp
from jax import lax
from jax.experimental import pallas as pl
from jax.experimental.pallas import tpu as pltpu
from jax.sharding import Mesh
from jax.sharding import PartitionSpec as P

FS = ("fs_0", "fs_1", "fs_2")
BF16, F32 = jnp.bfloat16, jnp.float32
MESH = pl.DeviceIdType.MESH

beta_one = 0.9
beta_two = 0.9
learn_rate = 0.01

N_FS, N_TP = 32, 4
TOKENS, D, RANK, COLS = 2048, 2048, 256, 256
ROWS = D // N_FS
TILES = D // 256
WIDTH = 3 * COLS
AHEAD = 3


def kernel(
    x, h, kc, vc, oc, wk, wv, wo, pk, pv, po, mk, mv, mo,
    step_k, step_v, step_o, copy_k, copy_v, copy_o, new_k, new_v, new_o,
    xbuf, cots, cots_t, grads, p_all, wm_all, wbuf, mbuf, parts, sums, total_buf,
    step_buf, new_buf, copy_buf, copy_t_buf,
    x_sem, cot_sem, p_sem, w_sem, out_sem,
    send_p, recv_p, pair_p, send_w, recv_w, pair_w,
    send_r, recv_r, send_g, recv_g, send_t, recv_t,
):
    z, y, c, t = (lax.axis_index(name) for name in (*FS, "tp"))
    me = (z * 4 + y) * 2 + c

    def device(da, db, core=0):
        zz = lax.rem(z + c * da + (1 - c) * db + 4, 4)
        yy = lax.rem(y + (1 - c) * da + c * db + 4, 4)
        return zz, yy, lax.rem(c + core, 2), t

    def block(da, db):
        zz, yy, cc, _ = device(da, db)
        return (zz * 4 + yy) * 2 + cc

    def remote(src, dst, send, recv, target):
        return pltpu.make_async_remote_copy(
            src_ref=src, dst_ref=dst, send_sem=send, recv_sem=recv,
            device_id=target, device_id_type=MESH,
        )

    barrier = pltpu.get_barrier_semaphore()
    for far in range(1, N_FS):
        other = lax.rem(me + far, N_FS)
        pl.semaphore_signal(
            barrier, inc=1, device_id=(other // 8, lax.rem(other // 2, 4), lax.rem(other, 2), t),
            device_id_type=MESH,
        )
    for far in range(1, N_TP):
        pl.semaphore_signal(
            barrier, inc=1, device_id=(z, y, c, lax.rem(t + far, N_TP)), device_id_type=MESH
        )

    def local(src, dst, sem):
        return pltpu.make_async_copy(src, dst, sem)

    p_in = [
        local(ref, p_all.at[me, :, pl.ds(k * COLS, COLS)], p_sem.at[k])
        for k, ref in enumerate((pk, pv, po))
    ]
    cot_in = [local(ref, cots.at[k], cot_sem.at[k]) for k, ref in enumerate((kc, vc, h))]
    w_in = [local(ref, wbuf.at[k], w_sem.at[k]) for k, ref in enumerate((wk, wv, wo))]
    m_in = [local(ref, mbuf.at[k], w_sem.at[3 + k]) for k, ref in enumerate((mk, mv, mo))]

    def tile_in(n):
        src = x if n < TILES else oc
        col = (n % TILES) * 256
        return local(src.at[:, pl.ds(col, 256)], xbuf.at[n], x_sem.at[n])

    for copy in (*p_in, *cot_in):
        copy.start()
    for n in range(AHEAD):
        tile_in(n).start()
    for copy in (*w_in, *m_in):
        copy.start()

    def transposed(k):
        cot_in[k].wait()
        for part in range(4):
            rows = pl.ds(part * 512, 512)
            cots_t[pl.ds(k * 256, 256), rows] = cots[k, rows, :].T

    def compute(n):
        tile_in(n).wait()
        if n + AHEAD < 2 * TILES:
            tile_in(n + AHEAD).start()
        lower, size = (0, 512) if n < TILES else (512, 256)
        made = jnp.dot(
            cots_t[pl.ds(lower, size), :], xbuf[n], preferred_element_type=F32
        )
        grads[pl.ds(lower, size), pl.ds((n % TILES) * 256, 256)] = made.astype(BF16)

    class Gather:
        def __init__(self, buf, split, send, recv, pair):
            self.buf, self.send, self.recv, self.pair = buf, send, recv, pair
            rows = buf.shape[1]
            self.part = {0: pl.ds(0, rows), 1: pl.ds(0, split), 2: pl.ds(split, rows - split)}
            self.slot = {("a", -1): 0, ("a", 1): 1, ("a2", 1): 2, ("a2", 2): 3}
            for i, da in enumerate((0, -1, 1, 2)):
                for j, key in enumerate((("b", da, -1), ("b", da, 1), ("b2", da, 1), ("b2", da, 2))):
                    self.slot[key] = 4 + 4 * i + j

        def go(self, offset, part, key, target):
            ref = self.buf.at[block(*offset), self.part[part], :]
            remote(ref, ref, self.send, self.recv.at[self.slot[key]], target).start()

        def pair_up(self, offset):
            ref = self.buf.at[block(*offset)]
            remote(ref, ref, self.send, self.pair, device(0, 0, 1)).start()

        def arrived(self, key, offset, part):
            ref = self.buf.at[block(*offset), self.part[part], :]
            remote(ref, ref, self.send, self.recv.at[self.slot[key]], device(0, 0, 1)).wait_recv()

        def both(self, da, offset):
            self.go(offset, 0, ("b", da, -1), device(0, 1))
            self.go(offset, 0, ("b", da, 1), device(0, -1))

        def on_b(self, da, side):
            self.arrived(("b", da, side), (da, side), 0)
            part = 1 if side < 0 else 2
            self.go((da, side), part, ("b2", da, part), device(0, -side))
            self.pair_up((da, side))

        def last_b(self, da):
            for part in (1, 2):
                self.arrived(("b2", da, part), (da, 2), part)
            self.pair_up((da, 2))

        def first(self):
            self.go((0, 0), 0, ("a", -1), device(1, 0))
            self.go((0, 0), 0, ("a", 1), device(-1, 0))
            self.both(0, (0, 0))
            self.pair_up((0, 0))

        def second(self):
            for side in (-1, 1):
                self.arrived(("a", side), (side, 0), 0)
                part = 1 if side < 0 else 2
                self.go((side, 0), part, ("a2", part), device(-side, 0))
            for side in (-1, 1):
                self.both(side, (side, 0))
                self.pair_up((side, 0))
            for side in (-1, 1):
                self.on_b(0, side)

        def third(self):
            for part in (1, 2):
                self.arrived(("a2", part), (2, 0), part)
            self.both(2, (2, 0))
            self.pair_up((2, 0))
            for da in (-1, 1):
                for side in (-1, 1):
                    self.on_b(da, side)
            self.last_b(0)

        def fourth(self):
            for side in (-1, 1):
                self.on_b(2, side)
            for da in (-1, 1):
                self.last_b(da)

        def fifth(self):
            self.last_b(2)

        def done(self):
            half = self.buf.at[pl.ds(0, 16)]
            remote(half, half, self.send, self.pair, device(0, 0, 1)).wait_recv()

        def drained(self):
            most = self.buf.at[pl.ds(0, 31)]
            remote(most, most, self.send, self.pair, device(0, 0, 1)).wait_send()

    factors = Gather(p_all, 32, send_p, recv_p, pair_p)
    states = Gather(wm_all, 48, send_w, recv_w, pair_w)

    transposed(0)
    transposed(1)
    pl.semaphore_wait(barrier, N_FS - 1 + N_TP - 1)
    for copy in p_in:
        copy.wait()
    factors.first()
    for n in range(7):
        compute(n)
    for copy in (*w_in, *m_in):
        copy.wait()
    for k in range(3):
        cols = pl.ds(k * COLS, COLS)
        wm_all[me, pl.ds(0, ROWS), cols] = wbuf[k].astype(BF16)
        wm_all[me, pl.ds(ROWS, 16), cols] = mbuf[k].reshape(16, COLS).astype(BF16)
    factors.second()
    compute(7)
    transposed(2)
    for n in range(TILES, 2 * TILES):
        compute(n)
    factors.third()
    factors.fourth()
    states.first()
    factors.fifth()
    factors.done()

    for k in range(3):
        cols = pl.ds(k * COLS, COLS)
        made = jnp.dot(
            grads[cols, :], p_all[:, :, cols].reshape(D, RANK), preferred_element_type=F32
        ).T
        stacked = jnp.concatenate(
            [made[:, :128].reshape(N_FS, 8, 128), made[:, 128:].reshape(N_FS, 8, 128)], axis=1
        )
        parts[0, :, pl.ds(k * 16, 16), :] = stacked.astype(BF16)

    def to_each(make):
        @pl.loop(1, N_FS)
        def _(far):
            other = lax.rem(me + far, N_FS)
            make(other, (other // 8, lax.rem(other // 2, 4), lax.rem(other, 2), t)).start()

    to_each(lambda other, target: remote(
        parts.at[0, other], parts.at[1, me], send_r, recv_r, target))
    states.second()
    rest = parts.at[1, pl.ds(0, N_FS - 1)]
    remote(rest, rest, send_r, recv_r, device(0, 0, 1)).wait_recv()
    parts[1, me] = parts[0, me]
    owned = jnp.sum(parts[1].astype(F32), axis=0)
    sums[me] = owned.astype(BF16)
    to_each(lambda other, target: remote(sums.at[me], sums.at[me], send_g, recv_g, target))
    states.third()
    rest = sums.at[pl.ds(0, N_FS - 1)]
    remote(rest, rest, send_g, recv_g, device(0, 0, 1)).wait_recv()

    wide = sums[...].astype(F32)
    squares = jnp.sum(jnp.sum((wide * wide).reshape(N_FS, 6, 8, 128), axis=0), axis=0)
    total_buf[t] = squares
    for far in range(1, N_TP):
        remote(
            total_buf.at[t], total_buf.at[t], send_t.at[far - 1], recv_t.at[far - 1],
            (z, y, c, lax.rem(t + far, N_TP)),
        ).start()
    states.fourth()
    for far in range(1, N_TP):
        remote(
            total_buf.at[t], total_buf.at[lax.rem(t + N_TP - far, N_TP)], send_t.at[far - 1],
            recv_t.at[far - 1], (z, y, c, lax.rem(t + far, N_TP)),
        ).wait_recv()
    total = jnp.sum(total_buf[0] + total_buf[1] + total_buf[2] + total_buf[3], keepdims=True)
    scale = 1.0 / jnp.sqrt(total / (3 * RANK * 4 * COLS) + 1e-06)
    states.fifth()

    outs = []
    for k, out in enumerate((new_k, new_v, new_o)):
        piece = owned[k * 16 : (k + 1) * 16]
        normed = jnp.concatenate([piece[:8], piece[8:]], axis=1) * scale
        new_buf[k, 0] = beta_one * mbuf[k, 0] + (1 - beta_one) * normed
        new_buf[k, 1] = beta_two * mbuf[k, 1] + (1 - beta_two) * normed * normed
        outs.append(local(new_buf.at[k], out, out_sem.at[k]))
        outs[-1].start()
    states.done()

    for k in range(3):
        cols = pl.ds(k * COLS, COLS)
        piece = sums[:, pl.ds(k * 16, 16), :].astype(F32)
        normed = jnp.concatenate([piece[:, :8], piece[:, 8:]], axis=2) * scale[:, :, None]
        old = wm_all[:, pl.ds(ROWS, 16), cols].astype(F32)
        moment_one = beta_one * old[:, :8] + (1 - beta_one) * normed
        moment_two = beta_two * old[:, 8:] + (1 - beta_two) * normed * normed
        direction = (moment_one * lax.rsqrt(moment_two)).reshape(RANK, COLS).astype(BF16)
        made = jnp.dot(p_all[me, :, cols], direction, preferred_element_type=F32)
        step_buf[k] = made
        outs.append(local(step_buf.at[k], (step_k, step_v, step_o)[k], out_sem.at[3 + k]))
        outs[-1].start()
        for part in range(4):
            rows = pl.ds(part * 8, 8)
            made = jnp.dot(
                p_all[rows, :, cols].reshape(512, RANK), direction, preferred_element_type=F32
            )
            fresh = wm_all[rows, pl.ds(0, ROWS), cols].reshape(512, COLS).astype(F32)
            fresh = fresh - learn_rate * made
            long = pl.ds(part * 512, 512)
            if k < 2:
                copy_buf[k, long, :] = fresh.astype(BF16)
                src, dst = copy_buf.at[k, long, :], (copy_k, copy_v)[k].at[long, :]
            else:
                copy_t_buf[:, long] = fresh.T.astype(BF16)
                src, dst = copy_t_buf.at[:, long], copy_o.at[:, long]
            outs.append(local(src, dst, out_sem.at[6 + k * 4 + part]))
            outs[-1].start()

    factors.drained()
    states.drained()
    rest = parts.at[0, pl.ds(0, N_FS - 1)]
    remote(rest, rest, send_r, recv_r, device(0, 0, 1)).wait_send()
    rest = sums.at[pl.ds(0, N_FS - 1)]
    remote(rest, rest, send_g, recv_g, device(0, 0, 1)).wait_send()
    for far in range(1, N_TP):
        remote(
            total_buf.at[t], total_buf.at[t], send_t.at[far - 1], recv_t.at[far - 1],
            (z, y, c, lax.rem(t + far, N_TP)),
        ).wait_send()
    for copy in outs:
        copy.wait()


def body(x, h, kc, vc, oc, wk, wv, wo, pk, pv, po, mk, mv, mo):
    anywhere = pl.BlockSpec(memory_space=pl.ANY)
    dma = pltpu.SemaphoreType.DMA
    outs = pl.pallas_call(
        kernel,
        out_shape=[
            *[jax.ShapeDtypeStruct((ROWS, COLS), F32)] * 3,
            *[jax.ShapeDtypeStruct((D, COLS), BF16)] * 2,
            jax.ShapeDtypeStruct((COLS, D), BF16),
            *[jax.ShapeDtypeStruct((2, 8, COLS), F32)] * 3,
        ],
        in_specs=[anywhere] * 14,
        out_specs=[anywhere] * 9,
        scratch_shapes=[
            pltpu.VMEM((2 * TILES, TOKENS, 256), BF16),
            pltpu.VMEM((3, TOKENS, COLS), BF16),
            pltpu.VMEM((WIDTH, TOKENS), BF16),
            pltpu.VMEM((WIDTH, D), BF16),
            pltpu.VMEM((N_FS, ROWS, WIDTH), BF16),
            pltpu.VMEM((N_FS, ROWS + 16, WIDTH), BF16),
            pltpu.VMEM((3, ROWS, COLS), F32),
            pltpu.VMEM((3, 2, 8, COLS), F32),
            pltpu.VMEM((2, N_FS, 48, 128), BF16),
            pltpu.VMEM((N_FS, 48, 128), BF16),
            pltpu.VMEM((N_TP, 8, 128), F32),
            pltpu.VMEM((3, ROWS, COLS), F32),
            pltpu.VMEM((3, 2, 8, COLS), F32),
            pltpu.VMEM((2, D, COLS), BF16),
            pltpu.VMEM((COLS, D), BF16),
            dma((2 * TILES,)), dma((3,)), dma((3,)), dma((6,)), dma((18,)),
            dma, dma((20,)), dma, dma, dma((20,)), dma,
            dma, dma, dma, dma, dma((3,)), dma((3,)),
        ],
        compiler_params=pltpu.CompilerParams(
            collective_id=0, has_side_effects=True, vmem_limit_bytes=60 * 2**20
        ),
    )(x, h, kc, vc, oc, wk, wv, wo.T, pk, pv, po, mk, mv, mo)
    step_k, step_v, step_o, *rest = outs
    return step_k, step_v, step_o.T, *rest


def solution(mesh):
    split = Mesh(mesh.devices.reshape(4, 4, 2, mesh.shape["tp"]), (*FS, "tp"))
    rows, both, cols = P(FS, None), P(FS, "tp"), P("tp", FS)
    moments = P(None, FS, "tp")
    return jax.shard_map(
        body,
        mesh=split,
        in_specs=(rows, both, both, both, rows, both, both, cols, rows, rows, rows, *[moments] * 3),
        out_specs=(
            both, both, cols, P(None, "tp"), P(None, "tp"), P("tp", None), *[moments] * 3
        ),
        check_vma=False,
    )
```

```python
import jax
import jax.numpy as jnp
from jax import lax
from jax.experimental import pallas as pl
from jax.experimental.pallas import tpu as pltpu
from jax.sharding import Mesh
from jax.sharding import PartitionSpec as P

FS = ("fs_0", "fs_1", "fs_2")
BF16, F32 = jnp.bfloat16, jnp.float32
MESH = pl.DeviceIdType.MESH

beta_one = 0.9
beta_two = 0.9
learn_rate = 0.01

N_FS, N_TP = 32, 4
TOKENS, D, RANK, COLS = 2048, 2048, 256, 256
ROWS = D // N_FS
TILES = D // 256
WIDTH = 3 * COLS
AHEAD = 4
SLOTS = AHEAD + 1


def exchange(
    x, h, kc, vc, oc, wk, wv, wo, pk, pv, po, mk, mv, mo,
    p_out, wm_out, sums_out, owned_out, scale_out,
    p_all, wm_all, sums, owned_buf, scale_buf,
    xbuf, cots, cots_t, grads, wbuf, mbuf, parts, total_buf,
    x_sem, cot_sem, p_sem, w_sem, out_sem,
    send_p, recv_p, pair_p, send_w, recv_w, pair_w,
    send_r, recv_r, send_g, recv_g, send_t, recv_t,
):
    z, y, c, t = (lax.axis_index(name) for name in (*FS, "tp"))
    me = (z * 4 + y) * 2 + c

    def device(da, db, core=0):
        zz = lax.rem(z + c * da + (1 - c) * db + 4, 4)
        yy = lax.rem(y + (1 - c) * da + c * db + 4, 4)
        return zz, yy, lax.rem(c + core, 2), t

    def block(da, db):
        zz, yy, cc, _ = device(da, db)
        return (zz * 4 + yy) * 2 + cc

    def remote(src, dst, send, recv, target):
        return pltpu.make_async_remote_copy(
            src_ref=src, dst_ref=dst, send_sem=send, recv_sem=recv,
            device_id=target, device_id_type=MESH,
        )

    barrier = pltpu.get_barrier_semaphore()
    for far in range(1, N_FS):
        other = lax.rem(me + far, N_FS)
        pl.semaphore_signal(
            barrier, inc=1, device_id=(other // 8, lax.rem(other // 2, 4), lax.rem(other, 2), t),
            device_id_type=MESH,
        )
    for far in range(1, N_TP):
        pl.semaphore_signal(
            barrier, inc=1, device_id=(z, y, c, lax.rem(t + far, N_TP)), device_id_type=MESH
        )

    def local(src, dst, sem):
        return pltpu.make_async_copy(src, dst, sem)

    p_in = [
        local(ref, p_all.at[me, :, pl.ds(k * COLS, COLS)], p_sem.at[k])
        for k, ref in enumerate((pk, pv, po))
    ]
    cot_in = [local(ref, cots.at[k], cot_sem.at[k]) for k, ref in enumerate((kc, vc, h))]
    w_in = [local(ref, wbuf.at[k], w_sem.at[k]) for k, ref in enumerate((wk, wv, wo))]
    m_in = [local(ref, mbuf.at[k], w_sem.at[3 + k]) for k, ref in enumerate((mk, mv, mo))]

    def tile_in(n):
        src = x if n < TILES else oc
        col = (n % TILES) * 256
        return local(src.at[:, pl.ds(col, 256)], xbuf.at[n % SLOTS], x_sem.at[n % SLOTS])

    for copy in (*p_in, *cot_in):
        copy.start()
    for n in range(AHEAD):
        tile_in(n).start()
    for copy in (*w_in, *m_in):
        copy.start()

    def transposed(k):
        cot_in[k].wait()
        for part in range(4):
            rows = pl.ds(part * 512, 512)
            cots_t[pl.ds(k * 256, 256), rows] = cots[k, rows, :].T

    def compute(n):
        tile_in(n).wait()
        if n + AHEAD < 2 * TILES:
            tile_in(n + AHEAD).start()
        lower, size = (0, 512) if n < TILES else (512, 256)
        made = jnp.dot(
            cots_t[pl.ds(lower, size), :], xbuf[n % SLOTS], preferred_element_type=F32
        )
        grads[pl.ds(lower, size), pl.ds((n % TILES) * 256, 256)] = made.astype(BF16)

    class Gather:
        def __init__(self, buf, split, send, recv, pair):
            self.buf, self.send, self.recv, self.pair = buf, send, recv, pair
            rows = buf.shape[1]
            self.part = {0: pl.ds(0, rows), 1: pl.ds(0, split), 2: pl.ds(split, rows - split)}
            self.slot = {("a", -1): 0, ("a", 1): 1, ("a2", 1): 2, ("a2", 2): 3}
            for i, da in enumerate((0, -1, 1, 2)):
                for j, key in enumerate((("b", da, -1), ("b", da, 1), ("b2", da, 1), ("b2", da, 2))):
                    self.slot[key] = 4 + 4 * i + j

        def go(self, offset, part, key, target):
            ref = self.buf.at[block(*offset), self.part[part], :]
            remote(ref, ref, self.send, self.recv.at[self.slot[key]], target).start()

        def pair_up(self, offset):
            ref = self.buf.at[block(*offset)]
            remote(ref, ref, self.send, self.pair, device(0, 0, 1)).start()

        def arrived(self, key, offset, part):
            ref = self.buf.at[block(*offset), self.part[part], :]
            remote(ref, ref, self.send, self.recv.at[self.slot[key]], device(0, 0, 1)).wait_recv()

        def both(self, da, offset):
            self.go(offset, 0, ("b", da, -1), device(0, 1))
            self.go(offset, 0, ("b", da, 1), device(0, -1))

        def on_b(self, da, side):
            self.arrived(("b", da, side), (da, side), 0)
            part = 1 if side < 0 else 2
            self.go((da, side), part, ("b2", da, part), device(0, -side))
            self.pair_up((da, side))

        def last_b(self, da):
            for part in (1, 2):
                self.arrived(("b2", da, part), (da, 2), part)
            self.pair_up((da, 2))

        def first(self):
            self.go((0, 0), 0, ("a", -1), device(1, 0))
            self.go((0, 0), 0, ("a", 1), device(-1, 0))
            self.both(0, (0, 0))
            self.pair_up((0, 0))

        def second(self):
            for side in (-1, 1):
                self.arrived(("a", side), (side, 0), 0)
                part = 1 if side < 0 else 2
                self.go((side, 0), part, ("a2", part), device(-side, 0))
            for side in (-1, 1):
                self.both(side, (side, 0))
                self.pair_up((side, 0))
            for side in (-1, 1):
                self.on_b(0, side)

        def third(self):
            for part in (1, 2):
                self.arrived(("a2", part), (2, 0), part)
            self.both(2, (2, 0))
            self.pair_up((2, 0))
            for da in (-1, 1):
                for side in (-1, 1):
                    self.on_b(da, side)
            self.last_b(0)

        def fourth(self):
            for side in (-1, 1):
                self.on_b(2, side)
            for da in (-1, 1):
                self.last_b(da)

        def fifth(self):
            self.last_b(2)

        def done(self):
            half = self.buf.at[pl.ds(0, 16)]
            remote(half, half, self.send, self.pair, device(0, 0, 1)).wait_recv()

        def drained(self):
            most = self.buf.at[pl.ds(0, 31)]
            remote(most, most, self.send, self.pair, device(0, 0, 1)).wait_send()

    factors = Gather(p_all, 32, send_p, recv_p, pair_p)
    states = Gather(wm_all, 48, send_w, recv_w, pair_w)

    transposed(0)
    transposed(1)
    pl.semaphore_wait(barrier, N_FS - 1 + N_TP - 1)
    for copy in p_in:
        copy.wait()
    factors.first()
    for n in range(7):
        compute(n)
    for copy in (*w_in, *m_in):
        copy.wait()
    for k in range(3):
        cols = pl.ds(k * COLS, COLS)
        wm_all[me, pl.ds(0, ROWS), cols] = wbuf[k].astype(BF16)
        wm_all[me, pl.ds(ROWS, 16), cols] = mbuf[k].reshape(16, COLS).astype(BF16)
    factors.second()
    compute(7)
    transposed(2)
    for n in range(TILES, 2 * TILES):
        compute(n)
    factors.third()
    factors.fourth()
    states.first()
    factors.fifth()
    factors.done()
    outs = [local(p_all, p_out, out_sem.at[0])]
    outs[-1].start()

    for k in range(3):
        cols = pl.ds(k * COLS, COLS)
        made = jnp.dot(
            grads[cols, :], p_all[:, :, cols].reshape(D, RANK), preferred_element_type=F32
        ).T
        stacked = jnp.concatenate(
            [made[:, :128].reshape(N_FS, 8, 128), made[:, 128:].reshape(N_FS, 8, 128)], axis=1
        )
        parts[0, :, pl.ds(k * 16, 16), :] = stacked.astype(BF16)

    def to_each(make):
        @pl.loop(1, N_FS)
        def _(far):
            other = lax.rem(me + far, N_FS)
            make(other, (other // 8, lax.rem(other // 2, 4), lax.rem(other, 2), t)).start()

    to_each(lambda other, target: remote(
        parts.at[0, other], parts.at[1, me], send_r, recv_r, target))
    states.second()
    rest = parts.at[1, pl.ds(0, N_FS - 1)]
    remote(rest, rest, send_r, recv_r, device(0, 0, 1)).wait_recv()
    parts[1, me] = parts[0, me]
    owned = jnp.sum(parts[1].astype(F32), axis=0)
    owned_buf[...] = owned
    sums[me] = owned.astype(BF16)
    to_each(lambda other, target: remote(sums.at[me], sums.at[me], send_g, recv_g, target))
    states.third()
    rest = sums.at[pl.ds(0, N_FS - 1)]
    remote(rest, rest, send_g, recv_g, device(0, 0, 1)).wait_recv()
    for n, (src, dst) in enumerate(((sums, sums_out), (owned_buf, owned_out))):
        outs.append(local(src, dst, out_sem.at[1 + n]))
        outs[-1].start()

    wide = sums[...].astype(F32)
    squares = jnp.sum(jnp.sum((wide * wide).reshape(N_FS, 6, 8, 128), axis=0), axis=0)
    total_buf[t] = squares
    for far in range(1, N_TP):
        remote(
            total_buf.at[t], total_buf.at[t], send_t.at[far - 1], recv_t.at[far - 1],
            (z, y, c, lax.rem(t + far, N_TP)),
        ).start()
    states.fourth()
    for far in range(1, N_TP):
        remote(
            total_buf.at[t], total_buf.at[lax.rem(t + N_TP - far, N_TP)], send_t.at[far - 1],
            recv_t.at[far - 1], (z, y, c, lax.rem(t + far, N_TP)),
        ).wait_recv()
    total = jnp.sum(total_buf[0] + total_buf[1] + total_buf[2] + total_buf[3], keepdims=True)
    scale_buf[...] = jnp.broadcast_to(1.0 / jnp.sqrt(total / (3 * RANK * 4 * COLS) + 1e-06), (8, 128))
    outs.append(local(scale_buf, scale_out, out_sem.at[3]))
    outs[-1].start()
    states.fifth()
    states.done()
    outs.append(local(wm_all, wm_out, out_sem.at[4]))
    outs[-1].start()


    factors.drained()
    states.drained()
    rest = parts.at[0, pl.ds(0, N_FS - 1)]
    remote(rest, rest, send_r, recv_r, device(0, 0, 1)).wait_send()
    rest = sums.at[pl.ds(0, N_FS - 1)]
    remote(rest, rest, send_g, recv_g, device(0, 0, 1)).wait_send()
    for far in range(1, N_TP):
        remote(
            total_buf.at[t], total_buf.at[t], send_t.at[far - 1], recv_t.at[far - 1],
            (z, y, c, lax.rem(t + far, N_TP)),
        ).wait_send()
    for copy in outs:
        copy.wait()


def update(
    p_in, wm_in, sums_in, owned_in, scale_in, mk, mv, mo,
    step_k, step_v, step_o, copy_k, copy_v, copy_o, new_k, new_v, new_o,
    p_all, wm_all, sums, owned, scale_buf, mbuf, step_buf, new_buf, copy_buf, copy_t_buf,
    in_sem, out_sem,
):
    z, y, c = (lax.axis_index(name) for name in FS)
    me = (z * 4 + y) * 2 + c
    rows_in, states_in = pl.ds(0, ROWS), pl.ds(ROWS, 16)
    first = [
        (sums_in, sums), (scale_in, scale_buf), (wm_in.at[:, states_in, :], wm_all.at[:, states_in, :]),
        (owned_in, owned), *[(ref, mbuf.at[k]) for k, ref in enumerate((mk, mv, mo))],
    ]
    for k in range(3):
        cols = pl.ds(k * COLS, COLS)
        first.append((p_in.at[:, :, cols], p_all.at[:, :, cols]))
        first.append((wm_in.at[:, rows_in, cols], wm_all.at[:, rows_in, cols]))
    loads = [pltpu.make_async_copy(*pair, in_sem.at[n]) for n, pair in enumerate(first)]
    for copy in loads:
        copy.start()
    for copy in loads[:7]:
        copy.wait()
    scale = scale_buf[pl.ds(0, 1), pl.ds(0, 1)]
    outs = []
    for k, out in enumerate((new_k, new_v, new_o)):
        piece = owned[pl.ds(k * 16, 16), :]
        normed = jnp.concatenate([piece[:8], piece[8:]], axis=1) * scale
        new_buf[k, 0] = beta_one * mbuf[k, 0] + (1 - beta_one) * normed
        new_buf[k, 1] = beta_two * mbuf[k, 1] + (1 - beta_two) * normed * normed
        outs.append(pltpu.make_async_copy(new_buf.at[k], out, out_sem.at[k]))
        outs[-1].start()

    for k in range(3):
        cols = pl.ds(k * COLS, COLS)
        piece = sums[:, pl.ds(k * 16, 16), :].astype(F32)
        normed = jnp.concatenate([piece[:, :8], piece[:, 8:]], axis=2) * scale[:, :, None]
        old = wm_all[:, pl.ds(ROWS, 16), cols].astype(F32)
        moment_one = beta_one * old[:, :8] + (1 - beta_one) * normed
        moment_two = beta_two * old[:, 8:] + (1 - beta_two) * normed * normed
        direction = (moment_one * lax.rsqrt(moment_two)).reshape(RANK, COLS).astype(BF16)
        loads[7 + 2 * k].wait()
        loads[8 + 2 * k].wait()
        made = jnp.dot(p_all[me, :, cols], direction, preferred_element_type=F32)
        step_buf[k] = made
        outs.append(pltpu.make_async_copy(step_buf.at[k], (step_k, step_v, step_o)[k], out_sem.at[3 + k]))
        outs[-1].start()
        for part in range(4):
            rows = pl.ds(part * 8, 8)
            made = jnp.dot(
                p_all[rows, :, cols].reshape(512, RANK), direction, preferred_element_type=F32
            )
            fresh = wm_all[rows, pl.ds(0, ROWS), cols].reshape(512, COLS).astype(F32)
            fresh = fresh - learn_rate * made
            long = pl.ds(part * 512, 512)
            if k < 2:
                copy_buf[k, long, :] = fresh.astype(BF16)
                src, dst = copy_buf.at[k, long, :], (copy_k, copy_v)[k].at[long, :]
            else:
                copy_t_buf[:, long] = fresh.T.astype(BF16)
                src, dst = copy_t_buf.at[:, long], copy_o.at[:, long]
            outs.append(pltpu.make_async_copy(src, dst, out_sem.at[6 + k * 4 + part]))
            outs[-1].start()

    for copy in outs:
        copy.wait()


def body(x, h, kc, vc, oc, wk, wv, wo, pk, pv, po, mk, mv, mo):
    anywhere = pl.BlockSpec(memory_space=pltpu.HBM)
    dma = pltpu.SemaphoreType.DMA
    held = pl.pallas_call(
        exchange,
        out_shape=[
            jax.ShapeDtypeStruct((N_FS, ROWS, WIDTH), BF16),
            jax.ShapeDtypeStruct((N_FS, ROWS + 16, WIDTH), BF16),
            jax.ShapeDtypeStruct((N_FS, 48, 128), BF16),
            jax.ShapeDtypeStruct((48, 128), F32),
            jax.ShapeDtypeStruct((8, 128), F32),
        ],
        in_specs=[anywhere] * 14,
        out_specs=[anywhere] * 5,
        scratch_shapes=[
            pltpu.VMEM((N_FS, ROWS, WIDTH), BF16),
            pltpu.VMEM((N_FS, ROWS + 16, WIDTH), BF16),
            pltpu.VMEM((N_FS, 48, 128), BF16),
            pltpu.VMEM((48, 128), F32),
            pltpu.VMEM((8, 128), F32),
            pltpu.VMEM((SLOTS, TOKENS, 256), BF16),
            pltpu.VMEM((3, TOKENS, COLS), BF16),
            pltpu.VMEM((WIDTH, TOKENS), BF16),
            pltpu.VMEM((WIDTH, D), BF16),
            pltpu.VMEM((3, ROWS, COLS), F32),
            pltpu.VMEM((3, 2, 8, COLS), F32),
            pltpu.VMEM((2, N_FS, 48, 128), BF16),
            pltpu.VMEM((N_TP, 8, 128), F32),
            dma((SLOTS,)), dma((3,)), dma((3,)), dma((6,)), dma((5,)),
            dma, dma((20,)), dma, dma, dma((20,)), dma,
            dma, dma, dma, dma, dma((3,)), dma((3,)),
        ],
        compiler_params=pltpu.CompilerParams(
            collective_id=0, has_side_effects=True, vmem_limit_bytes=63 * 2**20
        ),
    )(x, h, kc, vc, oc, wk, wv, wo.T, pk, pv, po, mk, mv, mo)
    step_k, step_v, step_o, *rest = pl.pallas_call(
        update,
        out_shape=[
            *[jax.ShapeDtypeStruct((ROWS, COLS), F32)] * 3,
            *[jax.ShapeDtypeStruct((D, COLS), BF16)] * 2,
            jax.ShapeDtypeStruct((COLS, D), BF16),
            *[jax.ShapeDtypeStruct((2, 8, COLS), F32)] * 3,
        ],
        in_specs=[anywhere] * 8,
        out_specs=[anywhere] * 9,
        scratch_shapes=[
            pltpu.VMEM((N_FS, ROWS, WIDTH), BF16),
            pltpu.VMEM((N_FS, ROWS + 16, WIDTH), BF16),
            pltpu.VMEM((N_FS, 48, 128), BF16),
            pltpu.VMEM((48, 128), F32),
            pltpu.VMEM((8, 128), F32),
            pltpu.VMEM((3, 2, 8, COLS), F32),
            pltpu.VMEM((3, ROWS, COLS), F32),
            pltpu.VMEM((3, 2, 8, COLS), F32),
            pltpu.VMEM((2, D, COLS), BF16),
            pltpu.VMEM((COLS, D), BF16),
            dma((13,)), dma((18,)),
        ],
        compiler_params=pltpu.CompilerParams(vmem_limit_bytes=63 * 2**20),
    )(*held, mk, mv, mo)
    return step_k, step_v, step_o.T, *rest


def solution(mesh):
    split = Mesh(mesh.devices.reshape(4, 4, 2, mesh.shape["tp"]), (*FS, "tp"))
    rows, both, cols = P(FS, None), P(FS, "tp"), P("tp", FS)
    moments = P(None, FS, "tp")
    return jax.shard_map(
        body,
        mesh=split,
        in_specs=(rows, both, both, both, rows, both, both, cols, rows, rows, rows, *[moments] * 3),
        out_specs=(
            both, both, cols, P(None, "tp"), P(None, "tp"), P("tp", None), *[moments] * 3
        ),
        check_vma=False,
    )
```

```python
import jax
import jax.numpy as jnp
from jax import lax
from jax.experimental import pallas as pl
from jax.experimental.pallas import tpu as pltpu
from jax.sharding import Mesh
from jax.sharding import PartitionSpec as P

FS = ("fs_0", "fs_1", "fs_2")
BF16, F32 = jnp.bfloat16, jnp.float32
MESH = pl.DeviceIdType.MESH

beta_one = 0.9
beta_two = 0.9
learn_rate = 0.01

N_FS, N_TP = 32, 4
TOKENS, D, RANK, COLS = 2048, 2048, 256, 256
ROWS = D // N_FS
TILE = 512
TILES = D // TILE
WIDTH = 3 * COLS
AHEAD = 3
SLOTS = AHEAD + 1


def exchange(
    x, h, kc, vc, oc, wk, wv, wo, pk, pv, po, mk, mv, mo,
    p_all, wm_all, sums, owned_buf, scale_buf,
    xbuf, cots, cots_t, grads, wbuf, mbuf, parts, pair_buf, half, ring_a, some, ring_b, total_buf,
    x_sem, cot_sem, p_sem, w_sem,
    send_p, recv_p, pair_p, send_w, recv_w, pair_w, step_send, step_recv,
):
    z, y, c, t = (lax.axis_index(name) for name in (*FS, "tp"))
    me = (z * 4 + y) * 2 + c

    def device(da, db, core=0):
        zz = lax.rem(z + c * da + (1 - c) * db + 4, 4)
        yy = lax.rem(y + (1 - c) * da + c * db + 4, 4)
        return zz, yy, lax.rem(c + core, 2), t

    def block(da, db):
        zz, yy, cc, _ = device(da, db)
        return (zz * 4 + yy) * 2 + cc

    def remote(src, dst, send, recv, target):
        return pltpu.make_async_remote_copy(
            src_ref=src, dst_ref=dst, send_sem=send, recv_sem=recv,
            device_id=target, device_id_type=MESH,
        )

    barrier = pltpu.get_barrier_semaphore()
    for far in range(1, N_FS):
        other = lax.rem(me + far, N_FS)
        pl.semaphore_signal(
            barrier, inc=1, device_id=(other // 8, lax.rem(other // 2, 4), lax.rem(other, 2), t),
            device_id_type=MESH,
        )
    for far in range(1, N_TP):
        for core in range(2):
            pl.semaphore_signal(
                barrier, inc=1, device_id=(z, y, core, lax.rem(t + far, N_TP)), device_id_type=MESH
            )

    def local(src, dst, sem):
        return pltpu.make_async_copy(src, dst, sem)

    p_in = [
        local(ref, p_all.at[me, :, pl.ds(k * COLS, COLS)], p_sem.at[k])
        for k, ref in enumerate((pk, pv, po))
    ]
    cot_in = [local(ref, cots.at[k], cot_sem.at[k]) for k, ref in enumerate((kc, vc, h))]
    w_in = [local(ref, wbuf.at[k], w_sem.at[k]) for k, ref in enumerate((wk, wv, wo))]
    m_in = [local(ref, mbuf.at[k], w_sem.at[3 + k]) for k, ref in enumerate((mk, mv, mo))]

    def tile_in(n):
        src = x if n < TILES else oc
        col = (n % TILES) * TILE
        return local(src.at[:, pl.ds(col, TILE)], xbuf.at[n % SLOTS], x_sem.at[n % SLOTS])

    for copy in (*p_in, *cot_in):
        copy.start()
    for n in range(AHEAD):
        tile_in(n).start()
    for copy in (*w_in, *m_in):
        copy.start()

    def transposed(k):
        cot_in[k].wait()
        for part in range(4):
            rows = pl.ds(part * 512, 512)
            cots_t[pl.ds(k * 256, 256), rows] = cots[k, rows, :].T

    def compute(n):
        tile_in(n).wait()
        if n + AHEAD < 2 * TILES:
            tile_in(n + AHEAD).start()
        lower, size = (0, 512) if n < TILES else (512, 256)
        made = jnp.dot(
            cots_t[pl.ds(lower, size), :], xbuf[n % SLOTS], preferred_element_type=F32
        )
        grads[pl.ds(lower, size), pl.ds((n % TILES) * TILE, TILE)] = made.astype(BF16)

    class Gather:
        def __init__(self, buf, split, send, recv, pair):
            self.buf, self.send, self.recv, self.pair = buf, send, recv, pair
            rows = buf.shape[1]
            self.part = {0: pl.ds(0, rows), 1: pl.ds(0, split), 2: pl.ds(split, rows - split)}
            self.slot = {("a", -1): 0, ("a", 1): 1, ("a2", 1): 2, ("a2", 2): 3}
            for i, da in enumerate((0, -1, 1, 2)):
                for j, key in enumerate((("b", da, -1), ("b", da, 1), ("b2", da, 1), ("b2", da, 2))):
                    self.slot[key] = 4 + 4 * i + j

        def go(self, offset, part, key, target):
            ref = self.buf.at[block(*offset), self.part[part], :]
            remote(ref, ref, self.send, self.recv.at[self.slot[key]], target).start()

        def pair_up(self, offset):
            ref = self.buf.at[block(*offset)]
            remote(ref, ref, self.send, self.pair, device(0, 0, 1)).start()

        def arrived(self, key, offset, part):
            ref = self.buf.at[block(*offset), self.part[part], :]
            remote(ref, ref, self.send, self.recv.at[self.slot[key]], device(0, 0, 1)).wait_recv()

        def both(self, da, offset):
            self.go(offset, 0, ("b", da, -1), device(0, 1))
            self.go(offset, 0, ("b", da, 1), device(0, -1))

        def on_b(self, da, side):
            self.arrived(("b", da, side), (da, side), 0)
            part = 1 if side < 0 else 2
            self.go((da, side), part, ("b2", da, part), device(0, -side))
            self.pair_up((da, side))

        def last_b(self, da):
            for part in (1, 2):
                self.arrived(("b2", da, part), (da, 2), part)
            self.pair_up((da, 2))

        def first(self):
            self.go((0, 0), 0, ("a", -1), device(1, 0))
            self.go((0, 0), 0, ("a", 1), device(-1, 0))
            self.both(0, (0, 0))
            self.pair_up((0, 0))

        def second(self):
            self.second_a()
            self.second_b()
            self.second_c()

        def third(self):
            self.third_a()
            self.third_b()

        def second_a(self):
            for side in (-1, 1):
                self.arrived(("a", side), (side, 0), 0)
                part = 1 if side < 0 else 2
                self.go((side, 0), part, ("a2", part), device(-side, 0))
            self.both(-1, (-1, 0))
            self.pair_up((-1, 0))

        def second_b(self):
            self.both(1, (1, 0))
            self.pair_up((1, 0))

        def second_c(self):
            for side in (-1, 1):
                self.on_b(0, side)

        def third_a(self):
            for part in (1, 2):
                self.arrived(("a2", part), (2, 0), part)
            self.both(2, (2, 0))
            self.pair_up((2, 0))

        def third_b(self):
            for da in (-1, 1):
                for side in (-1, 1):
                    self.on_b(da, side)
            self.last_b(0)

        def fourth(self):
            for side in (-1, 1):
                self.on_b(2, side)
            for da in (-1, 1):
                self.last_b(da)

        def fifth(self):
            self.last_b(2)

        def done(self):
            half = self.buf.at[pl.ds(0, 16)]
            remote(half, half, self.send, self.pair, device(0, 0, 1)).wait_recv()

        def drained(self):
            most = self.buf.at[pl.ds(0, 31)]
            remote(most, most, self.send, self.pair, device(0, 0, 1)).wait_send()

    factors = Gather(p_all, 32, send_p, recv_p, pair_p)
    states = Gather(wm_all, 48, send_w, recv_w, pair_w)

    transposed(0)
    transposed(1)
    pl.semaphore_wait(barrier, N_FS - 1 + 2 * (N_TP - 1))
    for copy in p_in:
        copy.wait()
    factors.first()
    for n in range(TILES):
        compute(n)
    for copy in (*w_in, *m_in):
        copy.wait()
    for k in range(3):
        cols = pl.ds(k * COLS, COLS)
        wm_all[me, pl.ds(0, ROWS), cols] = wbuf[k].astype(BF16)
        wm_all[me, pl.ds(ROWS, 16), cols] = mbuf[k].reshape(16, COLS).astype(BF16)
    factors.second()
    transposed(2)
    for n in range(TILES, 2 * TILES):
        compute(n)
    states.first()
    factors.third()
    factors.fourth()
    factors.fifth()
    factors.done()

    for k in range(3):
        cols = pl.ds(k * COLS, COLS)
        made = jnp.dot(
            grads[cols, :], p_all[:, :, cols].reshape(D, RANK), preferred_element_type=F32
        ).T
        left, right = (
            made[:, lane : lane + 128].reshape(16, 2, 8, 128) for lane in (0, 128)
        )
        stacked = jnp.concatenate([left, right], axis=2).astype(BF16)
        for core in range(2):
            parts[core, :, pl.ds(k * 16, 16), :] = stacked[:, core]

    def exchange_step(n, pairs):
        for src, dst, target in pairs:
            remote(src, dst, step_send.at[n], step_recv.at[n], target).start()

    def step_wait(n, like):
        remote(like, like, step_send.at[n], step_recv.at[n], device(0, 0, 1)).wait_recv()

    def step_sent(n, like):
        remote(like, like, step_send.at[n], step_recv.at[n], device(0, 0, 1)).wait_send()

    place_a, place_b = c * z + (1 - c) * y, c * y + (1 - c) * z

    def owner(pa, pb):
        return (c * pa + (1 - c) * pb) * 4 + c * pb + (1 - c) * pa

    near = lax.rem(c + 1, 2)
    exchange_step(0, [(parts.at[near], pair_buf, device(0, 0, 1))])
    states.second_a()
    step_wait(0, pair_buf)
    half[...] = (parts[c].astype(F32) + pair_buf[...].astype(F32)).astype(BF16)
    for far in range(1, 4):
        there = lax.rem(place_a + far, 4)
        exchange_step(1, [
            (half.at[owner(there, pb)], ring_a.at[far - 1, pb], device(far, 0)) for pb in range(4)
        ])
    states.second_b()
    step_wait(1, ring_a)
    for pb in range(4):
        some[pb] = (
            half[owner(place_a, pb)].astype(F32) + jnp.sum(ring_a[:, pb].astype(F32), axis=0)
        ).astype(BF16)
    exchange_step(2, [
        (some.at[lax.rem(place_b + far, 4)], ring_b.at[far - 1], device(0, far))
        for far in range(1, 4)
    ])
    states.second_c()
    step_wait(2, ring_b)
    owned = some[place_b].astype(F32) + jnp.sum(ring_b[...].astype(F32), axis=0)
    owned_buf[...] = owned
    mine = sums.at[c, owner(place_a, place_b)]
    mine[...] = owned.astype(BF16)
    exchange_step(3, [(mine, mine, device(far, 0)) for far in range(1, 4)])
    states.third_a()
    step_wait(3, ring_b)
    for far in range(1, 4):
        exchange_step(4, [
            (sums.at[c, owner(pa, place_b)], sums.at[c, owner(pa, place_b)], device(0, far))
            for pa in range(4)
        ])
    states.third_b()
    step_wait(4, ring_a)
    exchange_step(5, [(sums.at[c], sums.at[c], device(0, 0, 1))])

    wide = sums[c].astype(F32)
    place_t = c * N_TP + t
    total_buf[place_t] = jnp.sum(jnp.sum((wide * wide).reshape(16, 6, 8, 128), axis=0), axis=0)
    for far in range(1, 2 * N_TP):
        there = lax.rem(place_t + far, 2 * N_TP)
        exchange_step(6, [
            (total_buf.at[place_t], total_buf.at[place_t], (z, y, there // N_TP, lax.rem(there, N_TP)))
        ])
    states.fourth()
    step_wait(6, total_buf.at[pl.ds(0, 2 * N_TP - 1)])
    total = jnp.sum(jnp.sum(total_buf[...], axis=0), keepdims=True)
    scale_buf[...] = jnp.broadcast_to(
        1.0 / jnp.sqrt(total / (3 * RANK * N_TP * COLS) + 1e-06), (8, 128)
    )
    step_wait(5, pair_buf)
    states.fifth()
    states.done()

    factors.drained()
    states.drained()
    step_sent(0, pair_buf)
    step_sent(1, ring_a)
    step_sent(2, ring_b)
    step_sent(3, ring_b)
    step_sent(4, ring_a)
    step_sent(5, pair_buf)
    step_sent(6, total_buf.at[pl.ds(0, 2 * N_TP - 1)])


def update(
    p_all, wm_all, sums, owned, scale_buf, mk, mv, mo,
    step_k, step_v, step_o, copy_k, copy_v, copy_o, new_k, new_v, new_o,
    step_buf, new_buf, copy_buf, copy_t_buf, out_sem,
):
    z, y, c = (lax.axis_index(name) for name in FS)
    me = (z * 4 + y) * 2 + c
    mbuf = (mk, mv, mo)
    scale = scale_buf[pl.ds(0, 1), pl.ds(0, 1)]
    outs = []
    for k, out in enumerate((new_k, new_v, new_o)):
        piece = owned[pl.ds(k * 16, 16), :]
        normed = jnp.concatenate([piece[:8], piece[8:]], axis=1) * scale
        new_buf[k, 0] = beta_one * mbuf[k][0] + (1 - beta_one) * normed
        new_buf[k, 1] = beta_two * mbuf[k][1] + (1 - beta_two) * normed * normed
        outs.append(pltpu.make_async_copy(new_buf.at[k], out, out_sem.at[k]))
        outs[-1].start()

    for k in range(3):
        cols = pl.ds(k * COLS, COLS)
        piece = sums[:, :, pl.ds(k * 16, 16), :].astype(F32)
        piece = jnp.stack([piece[0], piece[1]], axis=1).reshape(N_FS, 16, 128)
        normed = jnp.concatenate([piece[:, :8], piece[:, 8:]], axis=2) * scale[:, :, None]
        old = wm_all[:, pl.ds(ROWS, 16), cols].astype(F32)
        moment_one = beta_one * old[:, :8] + (1 - beta_one) * normed
        moment_two = beta_two * old[:, 8:] + (1 - beta_two) * normed * normed
        direction = (moment_one * lax.rsqrt(moment_two)).reshape(RANK, COLS).astype(BF16)
        made = jnp.dot(p_all[me, :, cols], direction, preferred_element_type=F32)
        step_buf[k] = made
        outs.append(pltpu.make_async_copy(step_buf.at[k], (step_k, step_v, step_o)[k], out_sem.at[3 + k]))
        outs[-1].start()
        for part in range(4):
            rows = pl.ds(part * 8, 8)
            made = jnp.dot(
                p_all[rows, :, cols].reshape(512, RANK), direction, preferred_element_type=F32
            )
            fresh = wm_all[rows, pl.ds(0, ROWS), cols].reshape(512, COLS).astype(F32)
            fresh = fresh - learn_rate * made
            long = pl.ds(part * 512, 512)
            if k < 2:
                copy_buf[k, long, :] = fresh.astype(BF16)
                src, dst = copy_buf.at[k, long, :], (copy_k, copy_v)[k].at[long, :]
            else:
                copy_t_buf[:, long] = fresh.T.astype(BF16)
                src, dst = copy_t_buf.at[:, long], copy_o.at[:, long]
            outs.append(pltpu.make_async_copy(src, dst, out_sem.at[6 + k * 4 + part]))
            outs[-1].start()

    for copy in outs:
        copy.wait()


def body(x, h, kc, vc, oc, wk, wv, wo, pk, pv, po, mk, mv, mo):
    outside = pl.BlockSpec(memory_space=pltpu.HBM)
    inside = pl.BlockSpec(memory_space=pltpu.VMEM)
    dma = pltpu.SemaphoreType.DMA
    args = (x, h, kc, vc, oc, wk, wv, wo.T, pk, pv, po, mk, mv, mo)
    held = pl.pallas_call(
        exchange,
        out_shape=[
            pltpu.VMEM((N_FS, ROWS, WIDTH), BF16),
            pltpu.VMEM((N_FS, ROWS + 16, WIDTH), BF16),
            pltpu.VMEM((2, 16, 48, 128), BF16),
            pltpu.VMEM((48, 128), F32),
            pltpu.VMEM((8, 128), F32),
        ],
        in_specs=[outside] * 14,
        out_specs=[inside] * 5,
        scratch_shapes=[
            pltpu.VMEM((SLOTS, TOKENS, TILE), BF16),
            pltpu.VMEM((3, TOKENS, COLS), BF16),
            pltpu.VMEM((WIDTH, TOKENS), BF16),
            pltpu.VMEM((WIDTH, D), BF16),
            pltpu.VMEM((3, ROWS, COLS), F32),
            pltpu.VMEM((3, 2, 8, COLS), F32),
            pltpu.VMEM((2, 16, 48, 128), BF16),
            pltpu.VMEM((16, 48, 128), BF16),
            pltpu.VMEM((16, 48, 128), BF16),
            pltpu.VMEM((3, 4, 48, 128), BF16),
            pltpu.VMEM((4, 48, 128), BF16),
            pltpu.VMEM((3, 48, 128), BF16),
            pltpu.VMEM((2 * N_TP, 8, 128), F32),
            dma((SLOTS,)), dma((3,)), dma((3,)), dma((6,)),
            dma, dma((20,)), dma, dma, dma((20,)), dma, dma((7,)), dma((7,)),
        ],
        compiler_params=pltpu.CompilerParams(
            collective_id=0, has_side_effects=True, vmem_limit_bytes=42 * 2**20
        ),
    )(*(pltpu.with_memory_space_constraint(arg, pltpu.HBM) for arg in args))
    step_k, step_v, step_o, *rest = pl.pallas_call(
        update,
        out_shape=[
            *[jax.ShapeDtypeStruct((ROWS, COLS), F32)] * 3,
            *[jax.ShapeDtypeStruct((D, COLS), BF16)] * 2,
            jax.ShapeDtypeStruct((COLS, D), BF16),
            *[jax.ShapeDtypeStruct((2, 8, COLS), F32)] * 3,
        ],
        in_specs=[inside] * 8,
        out_specs=[outside] * 9,
        scratch_shapes=[
            pltpu.VMEM((3, ROWS, COLS), F32),
            pltpu.VMEM((3, 2, 8, COLS), F32),
            pltpu.VMEM((2, D, COLS), BF16),
            pltpu.VMEM((COLS, D), BF16),
            dma((18,)),
        ],
        compiler_params=pltpu.CompilerParams(vmem_limit_bytes=42 * 2**20),
    )(*held, mk, mv, mo)
    return step_k, step_v, step_o.T, *rest


def solution(mesh):
    split = Mesh(mesh.devices.reshape(4, 4, 2, mesh.shape["tp"]), (*FS, "tp"))
    rows, both, cols = P(FS, None), P(FS, "tp"), P("tp", FS)
    moments = P(None, FS, "tp")
    return jax.shard_map(
        body,
        mesh=split,
        in_specs=(rows, both, both, both, rows, both, both, cols, rows, rows, rows, *[moments] * 3),
        out_specs=(
            both, both, cols, P(None, "tp"), P(None, "tp"), P("tp", None), *[moments] * 3
        ),
        check_vma=False,
    )
```
